128 devices in a mesh: pp: 16 (over z, y), fs: 4 (over x), tp: 2 (over core).
Axes of the slice: x: 4, y: 4, z: 4, core: 2. Of those that a mesh axis runs over, the one named last changes fastest.
Arguments:
- tokens: bfloat16 [16, 8, 128, 2048], P('pp', ('fs', 'tp')), may hold values from -6 to 6
- layer_norm_scale: float32 [16, 2048], P('pp'), may hold values from 0.1 to 1.9
- input_weight: bfloat16 [16, 2048, 1024], P('pp'), may hold values from -0.125 to 0.125
- filter_weight: float32 [16, 4, 1024], P('pp'), may hold values from -3 to 3
- filter_bias: float32 [16, 1024], P('pp'), may hold values from -2 to 2
- recur_gate_weight: bfloat16 [16, 8, 128, 128], P('pp'), may hold values from -0.5 to 0.5
- recur_gate_bias: float32 [16, 1024], P('pp'), may hold values from -4 to 4
- input_gate_weight: bfloat16 [16, 8, 128, 128], P('pp'), may hold values from -0.5 to 0.5
- input_gate_bias: float32 [16, 1024], P('pp'), may hold values from -4 to 4
- decay_setting: float32 [16, 1024], P('pp'), may hold values from -2 to 8
- spike_log_decay: float32 [16, 128], P('pp'), may hold values from -0.7 to 0, as said below
- output_weight: bfloat16 [16, 1024, 2048], P('pp'), may hold values from -0.375 to 0.375
Outputs:
- result: bfloat16 [16, 8, 128, 2048], P('pp', ('fs', 'tp'))
The draws below stay inside these ranges and needn't reach their ends.
Inputs may be any that keep to these rules, and one draw needn't show every extreme that they name: `spike_log_decay`: zero at most positions; at a few positions of each layer drawn from the seed it lies between log(0.5) and log(0.8).
All inputs are finite; a program needn't handle non-finite values.
Results may differ from the reference program's by a relative error of at most 0.023.
Values may be sent and summed in bfloat16 or wider, within the bound.
No kernel may reach another device: no remote copies, remote signals or barrier semaphores. Data moves between devices by JAX's collectives and lax.ppermute only.
A program may use at most 64 MiB of HBM per device.

```python
import math
import jax
import jax.numpy as jnp
from jax import lax

D = 2048
RW = 1024
GB = 8
BW = 128
CONV = 4
LEN = 128
SECTIONS = 16
MICRO = 16
SEQS = 8


def draw_spike_log_decay(key, part):
    marks = jax.random.randint(jax.random.fold_in(key, 11), (SECTIONS, LEN), 0, LEN) < 3
    values = jax.random.uniform(jax.random.fold_in(key, 12), (SECTIONS, LEN), jnp.float32, math.log(0.5), math.log(0.8))
    return jnp.where(marks, values, 0.0).astype(jnp.float32)


def draw_decay_setting(key, part):
    fast_share = 0.6
    fast_low = -1.5
    fast_high = 0.5
    picks = jax.random.uniform(jax.random.fold_in(key, 21), (SECTIONS, RW), jnp.float32)
    quick = jax.random.uniform(jax.random.fold_in(key, 22), (SECTIONS, RW), jnp.float32, fast_low, fast_high)
    slow = jax.random.uniform(jax.random.fold_in(key, 23), (SECTIONS, RW), jnp.float32, 6.0, 8.0)
    return jnp.where(picks < fast_share, quick, slow).astype(jnp.float32)


def steps_of(stream_key, dims, split, least, largest):
    loudness = 1.0
    for position, parts in split:
        draws = jax.random.uniform(jax.random.fold_in(jax.random.fold_in(stream_key, 6), position), (parts,), jnp.float32, least / len(split), largest / len(split))
        loudness = loudness * jnp.repeat(jnp.exp(draws), dims[position] // parts).reshape((-1,) + (1,) * (len(dims) - 1 - position))
    return loudness


def bell_draw(stream_key, dims, spread, limit, shards=(), kind=jnp.bfloat16):
    drawn = spread * jax.random.normal(stream_key, dims, jnp.float32)
    if shards:
        drawn = drawn * steps_of(stream_key, dims, shards, -0.22, 0.18)
    return jnp.clip(drawn, -limit, limit).astype(kind)


def setup_inputs(seed: int = 0) -> dict:
    arg_keys = jax.random.split(jax.random.key(seed), 13)
    tokens = bell_draw(arg_keys[0], (MICRO, SEQS, LEN, D), 1.0, 6.0, ((0, 16), (1, 8)))
    layer_norm_scale = jnp.clip(1.0 + 0.18 * jax.random.normal(arg_keys[1], (SECTIONS, D), jnp.float32), 0.1, 1.9)
    input_weight = bell_draw(arg_keys[2], (SECTIONS, D, RW), D ** -0.5, 0.125, ((0, 16),))
    filter_weight = bell_draw(arg_keys[3], (SECTIONS, CONV, RW), CONV ** -0.5, 3.0, ((0, 16),), jnp.float32)
    filter_bias = bell_draw(arg_keys[4], (SECTIONS, RW), 0.3, 2.0, ((0, 16),), jnp.float32)
    recur_gate_weight = bell_draw(arg_keys[5], (SECTIONS, GB, BW, BW), BW ** -0.5, 0.5, ((0, 16),))
    recur_gate_bias = bell_draw(arg_keys[6], (SECTIONS, RW), 1.0, 4.0, ((0, 16),), jnp.float32)
    input_gate_weight = bell_draw(arg_keys[7], (SECTIONS, GB, BW, BW), BW ** -0.5, 0.5, ((0, 16),))
    input_gate_bias = bell_draw(arg_keys[8], (SECTIONS, RW), 1.0, 4.0, ((0, 16),), jnp.float32)
    decay_setting = draw_decay_setting(jax.random.fold_in(arg_keys[12], 71), 0)
    spike_log_decay = draw_spike_log_decay(jax.random.fold_in(arg_keys[12], 71), 0)
    output_weight = bell_draw(arg_keys[11], (SECTIONS, RW, D), (RW // 4) ** -0.5, 0.375, ((0, 16),))
    return {"tokens": tokens, "layer_norm_scale": layer_norm_scale, "input_weight": input_weight, "filter_weight": filter_weight, "filter_bias": filter_bias, "recur_gate_weight": recur_gate_weight, "recur_gate_bias": recur_gate_bias, "input_gate_weight": input_gate_weight, "input_gate_bias": input_gate_bias, "decay_setting": decay_setting, "spike_log_decay": spike_log_decay, "output_weight": output_weight}


def combine_pair(left, right):
    return (left[0] * right[0], right[0] * left[1] + right[1])

def one_layer(hidden, weight_bundle):
    norm_factor, input_projected, filter_kernel_taps, filter_offset, retention_weight, retention_bias, injection_weight, injection_bias, unscaled_decay, decay_spike, output_projected = weight_bundle
    batch = hidden.shape[0]
    width = input_projected.shape[1]
    taps = filter_kernel_taps.shape[0]
    blocks = retention_weight.shape[0]
    hidden32 = hidden.astype(jnp.float32)
    squares = lax.optimization_barrier(jnp.mean(hidden32 * hidden32, axis=-1, keepdims=True))
    normed = (hidden32 * lax.rsqrt(squares + 1e-06) * norm_factor).astype(jnp.bfloat16)
    mixed_in = jnp.dot(normed.reshape(-1, normed.shape[-1]), input_projected, preferred_element_type=jnp.float32)
    mixed_in = mixed_in.astype(jnp.bfloat16).reshape(batch, -1, width)
    length = mixed_in.shape[1]
    padded = jnp.pad(mixed_in.astype(jnp.float32), ((0, 0), (taps - 1, 0), (0, 0)))
    conv_out = filter_offset + sum((padded[:, k:k + length] * filter_kernel_taps[k] for k in range(taps)))
    conv_out = conv_out.astype(jnp.bfloat16)
    grouped = conv_out.astype(jnp.float32).reshape(batch * length, blocks, -1)
    retention_gate = jax.nn.sigmoid(jnp.einsum('ngi,gij->ngj', grouped, retention_weight.astype(jnp.float32)).reshape(batch, length, width) + retention_bias)
    inject = jax.nn.sigmoid(jnp.einsum('ngi,gij->ngj', grouped, injection_weight.astype(jnp.float32)).reshape(batch, length, width) + injection_bias)
    decay_logarithm = -8.0 * retention_gate * jax.nn.softplus(-unscaled_decay) + decay_spike[None, :, None]
    decay = jnp.exp(decay_logarithm)
    update = jnp.sqrt(-jnp.expm1(2.0 * decay_logarithm)) * inject * conv_out.astype(jnp.float32)
    states = lax.associative_scan(combine_pair, (decay, update), axis=1)[1].astype(jnp.bfloat16)
    projected = jnp.dot(states.reshape(-1, width), output_projected, preferred_element_type=jnp.float32)
    return (hidden32 + projected.reshape(hidden.shape)).astype(jnp.bfloat16)

def reference(tokens, layer_norm_scale, input_weight, filter_weight, filter_bias, recur_gate_weight, recur_gate_bias, input_gate_weight, input_gate_bias, decay_setting, spike_log_decay, output_weight):
    hidden = tokens.reshape(-1, tokens.shape[2], tokens.shape[3])

    def advance(carry, weight_bundle):
        return (one_layer(carry, weight_bundle), None)
    layer_stacked_params = (layer_norm_scale, input_weight, filter_weight, filter_bias, recur_gate_weight, recur_gate_bias, input_gate_weight, input_gate_bias, decay_setting, spike_log_decay, output_weight)
    hidden, unused = lax.scan(advance, hidden, layer_stacked_params)
    return hidden.reshape(tokens.shape)
```

```python
import numpy as np
import jax
import jax.numpy as jnp
from jax import lax
from jax.experimental import pallas as pl
from jax.experimental.pallas import tpu as pltpu
from jax.sharding import Mesh, PartitionSpec as P

F32 = jnp.float32
BF16 = jnp.bfloat16
STAGES = 4
LAYERS = 4
CHUNK = 64
D = 2048
RW = 1024
TILE = 256
PAYLOAD = 544
STATE = 32


def load_kernel(source, target, sem):
    copies = [
        pltpu.make_async_copy(source.at[i], target.at[i], sem.at[i])
        for i in range(LAYERS)
    ]
    for copy in copies:
        copy.start()
    for copy in copies:
        copy.wait()


def load_weights(gathered):
    return pl.pallas_call(
        load_kernel,
        in_specs=[pl.BlockSpec(memory_space=pltpu.HBM)],
        out_specs=pl.BlockSpec(memory_space=pltpu.VMEM),
        out_shape=pltpu.VMEM((LAYERS, 8, PAYLOAD, RW), BF16),
        scratch_shapes=[pltpu.SemaphoreType.DMA((LAYERS,))],
        compiler_params=pltpu.CompilerParams(vmem_limit_bytes=4 * 2**20),
        name="load_weights",
    )(gathered)


def rolled(value):
    return pltpu.roll(value, 1, axis=0)


def layer(index, first, weights, params, spikes, state_in, state_out, hidden, normed, states):
    rows = CHUNK // 8
    sub = lax.broadcasted_iota(jnp.int32, (8, TILE), 0)
    top = sub == 0
    total = jnp.zeros((CHUNK, 128), F32)
    for j in range(D // 128):
        part = hidden[:, j * 128 : (j + 1) * 128].astype(F32)
        total = total + part * part
    scale = lax.rsqrt(jnp.sum(total, axis=1, keepdims=True) * (1.0 / D) + 1e-6)
    for e in range(8):
        cols = slice(e * TILE, (e + 1) * TILE)
        gain = params[index, e // 4 : e // 4 + 1, (e % 4) * TILE : (e % 4 + 1) * TILE]
        normed[:, cols] = (hidden[:, cols].astype(F32) * scale * gain).astype(BF16)
    for n in range(4):
        cols = slice(n * TILE, (n + 1) * TILE)
        mixed = None
        for e in range(8):
            part = jnp.dot(
                normed[:, e * TILE : (e + 1) * TILE],
                weights[index, e, 0:TILE, cols],
                preferred_element_type=F32,
            )
            mixed = part if mixed is None else mixed + part
        mixed = mixed.astype(BF16).astype(F32)
        at = [mixed[r * 8 : (r + 1) * 8] for r in range(rows)]
        before = []
        for j in range(3):
            turn = rolled(at[rows - 3 + j])
            kept = jnp.where(first, 0.0, state_in[index, 8 + 8 * j : 16 + 8 * j, cols])
            before.append(jnp.where(top, kept, turn))
            state_out[index, 8 + 8 * j : 16 + 8 * j, cols] = turn
        line = before + at
        taps = [params[index, 2 + k : 3 + k, cols] for k in range(4)]
        bias = params[index, 6:7, cols]
        conv = [
            (
                bias
                + (
                    (line[r] * taps[0] + line[r + 1] * taps[1])
                    + (line[r + 2] * taps[2] + line[r + 3] * taps[3])
                )
            )
            for r in range(rows)
        ]
        conv = jnp.concatenate(conv, axis=0).astype(BF16)
        recur = []
        inject = []
        for b in range(2):
            block = 2 * n + b
            gate = jnp.concatenate(
                [
                    weights[index, block, 2 * TILE : PAYLOAD, q * TILE : (q + 1) * TILE]
                    for q in range(4)
                ],
                axis=0,
            )
            both = jnp.dot(
                conv[:, b * 128 : (b + 1) * 128], gate, preferred_element_type=F32
            )
            recur.append(both[:, :128])
            inject.append(both[:, 128:])
        recur = jnp.concatenate(recur, axis=1)
        inject = jnp.concatenate(inject, axis=1)
        conv = conv.astype(F32)
        recur_bias = params[index, 7:8, cols]
        inject_bias = params[index, 8:9, cols]
        speed = params[index, 9:10, cols]
        state = None
        local_state = []
        local_decay = []
        for r in range(rows):
            here = slice(r * 8, (r + 1) * 8)
            spike = spikes[index, here, :]
            spike = jnp.concatenate([spike, spike], axis=1)
            y = speed * jnp.tanh(recur[here] + recur_bias) + (speed - spike)
            t = jnp.tanh(y)
            decay = jnp.exp(-y)
            twice = t + t
            root = t * lax.rsqrt(jnp.maximum(twice + twice * t, 1e-37))
            value = conv[here]
            update = root * (value + value * jnp.tanh(inject[here] + inject_bias))
            if r == 0:
                local_state.append(update)
                local_decay.append(decay)
            else:
                local_state.append(decay * local_state[-1] + update)
                local_decay.append(decay * local_decay[-1])
        a = local_decay[-1]
        h = local_state[-1]
        for shift in (1, 2, 4):
            far = sub < shift
            a_back = jnp.where(far, 1.0, pltpu.roll(a, shift, axis=0))
            h_back = jnp.where(far, 0.0, pltpu.roll(h, shift, axis=0))
            h = a * h_back + h
            a = a * a_back
        start = jnp.where(first, 0.0, state_in[index, 0:8, cols])
        start = jnp.broadcast_to(start[7:8], (8, TILE))
        ends = a * start + h
        state_out[index, 0:8, cols] = ends
        carry = jnp.where(top, start, rolled(ends))
        states[:, cols] = jnp.concatenate(
            [local_state[r] + local_decay[r] * carry for r in range(rows)], axis=0
        ).astype(BF16)
    for e in range(8):
        cols = slice(e * TILE, (e + 1) * TILE)
        out = None
        for k in range(4):
            part = jnp.dot(
                states[:, k * TILE : (k + 1) * TILE],
                weights[index, e, TILE : 2 * TILE, k * TILE : (k + 1) * TILE],
                preferred_element_type=F32,
            )
            out = part if out is None else out + part
        hidden[:, cols] = (hidden[:, cols].astype(F32) + out).astype(BF16)


def stage_kernel(
    flags, fresh, passed, weights, params, spikes, state_in, out, state_out, normed, states
):
    @pl.when(flags[0] == 1)
    def _():
        first = flags[2] == 1

        @pl.when(flags[1] == 1)
        def _():
            out[...] = fresh[...]

        @pl.when(flags[1] == 0)
        def _():
            out[...] = passed[...]

        def body(index, unused):
            layer(
                index, first, weights, params, spikes, state_in, state_out, out, normed, states
            )
            return unused

        lax.fori_loop(0, LAYERS, body, 0)


def run_stage(flags, fresh, passed, weights, params, spikes, state):
    vmem = pl.BlockSpec(memory_space=pltpu.VMEM)
    flops = LAYERS * CHUNK * 2 * (2 * D * RW + 2 * RW * 128)
    return pl.pallas_call(
        stage_kernel,
        in_specs=[pl.BlockSpec(memory_space=pltpu.SMEM)] + [vmem] * 6,
        out_specs=[vmem, vmem],
        out_shape=[
            jax.ShapeDtypeStruct((CHUNK, D), BF16),
            jax.ShapeDtypeStruct((LAYERS, STATE, RW), F32),
        ],
        scratch_shapes=[pltpu.VMEM((CHUNK, D), BF16), pltpu.VMEM((CHUNK, RW), BF16)],
        compiler_params=pltpu.CompilerParams(vmem_limit_bytes=14 * 2**20),
        cost_estimate=pl.CostEstimate(
            flops=4 * flops, transcendentals=5 * LAYERS * CHUNK * RW, bytes_accessed=2**20
        ),
        name="stage",
    )(flags, fresh, passed, weights, params, spikes, state)


def shifted(value, by):
    return lax.ppermute(value, "z", [(i, (i + by) % STAGES) for i in range(STAGES)])


def turned(value):
    rows = CHUNK // 8
    halves = value.shape[0] // CHUNK
    return value.reshape(halves, 8, rows, -1).swapaxes(1, 2).reshape(value.shape)


def unturned(value):
    rows = CHUNK // 8
    halves = value.shape[0] // CHUNK
    return value.reshape(halves, rows, 8, -1).swapaxes(1, 2).reshape(value.shape)


def local(
    tokens,
    layer_norm_scale,
    input_weight,
    filter_weight,
    filter_bias,
    recur_gate_weight,
    recur_gate_bias,
    input_gate_weight,
    input_gate_bias,
    decay_setting,
    spike_log_decay,
    output_weight,
):
    stage = lax.axis_index("z")
    piece = lax.axis_index(("fs", "tp"))
    half = jnp.asarray(0.5, BF16)

    w_in = lax.dynamic_slice(input_weight[0], (piece * TILE, 0), (TILE, RW))
    w_out = lax.dynamic_slice(output_weight[0], (0, piece * TILE), (RW, TILE))
    w_out = jnp.concatenate([w_out[k * TILE : (k + 1) * TILE] for k in range(4)], axis=1)
    gates = jnp.concatenate(
        [
            lax.dynamic_index_in_dim(recur_gate_weight[0], piece, 0, keepdims=False),
            lax.dynamic_index_in_dim(input_gate_weight[0], piece, 0, keepdims=False),
        ],
        axis=1,
    ) * half
    gates = jnp.concatenate([gates[q * 32 : (q + 1) * 32] for q in range(4)], axis=1)
    payload = jnp.concatenate([w_in, w_out, gates], axis=0)
    gathered = lax.all_gather(payload, ("y", "fs", "tp"), axis=0, tiled=True)
    gathered = gathered.reshape(LAYERS, 8, PAYLOAD, RW)

    small = jnp.concatenate(
        [
            layer_norm_scale.reshape(2, RW),
            filter_weight[0],
            filter_bias,
            0.5 * recur_gate_bias,
            0.5 * input_gate_bias,
            4.0 * jax.nn.softplus(-decay_setting),
            jnp.pad(spike_log_decay, ((0, 0), (0, RW - spike_log_decay.shape[1]))),
            jnp.zeros((5, RW), F32),
        ],
        axis=0,
    )
    params = lax.all_gather(small[None], "y", axis=0, tiled=True)
    spikes = params[:, 10, : tokens.shape[2]]
    spikes = spikes.reshape(LAYERS, 2, 8, CHUNK // 8).swapaxes(2, 3).reshape(LAYERS, 2, CHUNK, 1)
    spikes = jnp.broadcast_to(spikes, (LAYERS, 2, CHUNK, 128))
    spikes = [spikes[:, 0], spikes[:, 1]]

    mine = turned(tokens[0, 0])
    batches = [mine] + [shifted(mine, -by) for by in range(1, STAGES)]
    weights = load_weights(gathered)

    chunks = 2 * STAGES
    steps = chunks + 2 * (STAGES - 1)
    state = jnp.zeros((LAYERS, STATE, RW), F32)
    results = []
    received = []
    for t in range(steps):
        chunk = t - 2 * stage
        active = (chunk >= 0) & (chunk < chunks)
        flags = jnp.stack([active, stage == 0, jnp.asarray(t % 2 == 0)]).astype(jnp.int32)
        batch = batches[min(t // 2, STAGES - 1)]
        fresh = batch[:CHUNK] if t % 2 == 0 else batch[CHUNK:]
        passed = received[t - 2] if t >= 2 else fresh
        result, state = run_stage(
            flags, fresh, passed, weights, params, spikes[t % 2], state
        )
        results.append(result)
        received.append(shifted(result, 1) if t < steps - 2 else None)

    last = 2 * (STAGES - 1)
    halves = []
    for j in range(2):
        home = [received[last + j]]
        home += [shifted(results[last + 2 * m + j], -(STAGES - 1 - m)) for m in range(1, STAGES - 1)]
        home += [results[last + 2 * (STAGES - 1) + j]]
        chosen = home[0]
        for m in range(1, STAGES):
            chosen = jnp.where(stage == m, home[m], chosen)
        halves.append(chosen)
    return unturned(jnp.concatenate(halves, axis=0))[None, None]


def solution(mesh):
    split = Mesh(mesh.devices.reshape(4, 4, 4, 2), ("z", "y", "fs", "tp"))
    layers = ("z", "y")
    placed = (
        P(layers, ("fs", "tp"), None, None),
        P(layers, None),
        P(layers, None, None),
        P(layers, None, None),
        P(layers, None),
        P(layers, None, None, None),
        P(layers, None),
        P(layers, None, None, None),
        P(layers, None),
        P(layers, None),
        P(layers, None),
        P(layers, None, None),
    )
    return jax.shard_map(
        local,
        mesh=split,
        in_specs=placed,
        out_specs=P(layers, ("fs", "tp"), None, None),
        check_vma=False,
    )
```

```python
import jax
import jax.numpy as jnp
from jax import lax
from jax.experimental import pallas as pl
from jax.experimental.pallas import tpu as pltpu
from jax.sharding import Mesh, PartitionSpec as P


F32 = jnp.float32
BF16 = jnp.bfloat16
STAGES = 4
LAYERS = 4
CHUNK = 64
D = 2048
RW = 1024
TILE = 256
REST = 288
STATE = 32


def copy_all(copies):
    for copy in copies:
        copy.start()
    for copy in copies:
        copy.wait()


def in_kernel(where, own, one, one_other, three, three_other, two, two_other, target, sem):
    copies = [
        (own.at[0, pl.ds(e * TILE, TILE)], target.at[0, e])
        for e in range(8)
    ]
    for slot, mine, other in ((1, one, one_other), (3, three, three_other), (2, two, two_other)):
        for core, source in ((0, mine), (1, other)):
            for q in range(4):
                copies.append((source.at[q], target.at[slot, 2 * q + (where[1] ^ core)]))
    copy_all([pltpu.make_async_copy(source, target, sem) for source, target in copies])


def out_kernel(where, own, gates, near, near_other, far, far_other, target, sem):
    copies = []
    for e in range(8):
        copies.append((gates.at[e], target.at[0, e, pl.ds(TILE, REST - TILE)]))
        for k in range(4):
            there = pl.ds(k * TILE, TILE)
            copies.append(
                (
                    own.at[0, there, pl.ds(e * TILE, TILE)],
                    target.at[0, e, pl.ds(0, TILE), there],
                )
            )
    for core, nears, fars in ((0, near, far), (1, near_other, far_other)):
        for i, mask in enumerate((0, 1, 3, 2)):
            e = 2 * (where[0] ^ mask) + (where[1] ^ core)
            copies.append((nears.at[2 * i], target.at[1, e]))
            copies.append((nears.at[2 * i + 1], target.at[3, e]))
            copies.append((fars.at[i], target.at[2, e]))
    copy_all([pltpu.make_async_copy(source, target, sem) for source, target in copies])


def load(kernel, rows, where, *sources):
    return pl.pallas_call(
        kernel,
        in_specs=[pl.BlockSpec(memory_space=pltpu.SMEM)]
        + [pl.BlockSpec(memory_space=pltpu.HBM)] * len(sources),
        out_specs=pl.BlockSpec(memory_space=pltpu.VMEM),
        out_shape=pltpu.VMEM((LAYERS, 8, rows, RW), BF16),
        scratch_shapes=[pltpu.SemaphoreType.DMA],
        compiler_params=pltpu.CompilerParams(vmem_limit_bytes=2 * 2**20),
        name="load_weights",
    )(where, *[pltpu.with_memory_space_constraint(source, pltpu.HBM) for source in sources])


def crossed(value, axis, mask):
    return lax.ppermute(value, axis, [(i, i ^ mask) for i in range(lax.axis_size(axis))])


def ring_gather(value, axis):
    cut = value.shape[0] // 2
    one = crossed(value, axis, 1)
    three = crossed(value, axis, 3)
    low = crossed(one[:cut], axis, 3)
    high = crossed(three[cut:], axis, 1)
    return one, three, low, high


def rolled(value):
    return pltpu.roll(value, 1, axis=0)


def layer(slot, first, w_in, w_out, params, spikes, state_in, state_out, hidden, normed, states):
    rows = CHUNK // 8
    sub = lax.broadcasted_iota(jnp.int32, (8, TILE), 0)
    top = sub == 0
    total = jnp.zeros((CHUNK, 128), F32)
    for j in range(D // 128):
        part = hidden[:, j * 128 : (j + 1) * 128].astype(F32)
        total = total + part * part
    scale = lax.rsqrt(jnp.sum(total, axis=1, keepdims=True) * (1.0 / D) + 1e-6)
    for e in range(8):
        cols = slice(e * TILE, (e + 1) * TILE)
        gain = params[slot, e // 4 : e // 4 + 1, (e % 4) * TILE : (e % 4 + 1) * TILE]
        normed[:, cols] = (hidden[:, cols].astype(F32) * scale * gain).astype(BF16)
    wide = 2 * TILE

    def project(p):
        acc = None
        for e in range(8):
            part = jnp.dot(
                normed[:, e * TILE : (e + 1) * TILE],
                w_in[slot, e, :, p * wide : (p + 1) * wide],
                preferred_element_type=F32,
            )
            acc = part if acc is None else acc + part
        return acc

    def convolve(p, mixed):
        pieces = []
        for n in (2 * p, 2 * p + 1):
            cols = slice(n * TILE, (n + 1) * TILE)
            here = mixed[:, (n % 2) * TILE : (n % 2 + 1) * TILE].astype(BF16).astype(F32)
            at = [here[r * 8 : (r + 1) * 8] for r in range(rows)]
            before = []
            for j in range(3):
                turn = rolled(at[rows - 3 + j])
                kept = jnp.where(first, 0.0, state_in[slot, 8 + 8 * j : 16 + 8 * j, cols])
                before.append(jnp.where(top, kept, turn))
                state_out[slot, 8 + 8 * j : 16 + 8 * j, cols] = turn
            line = before + at
            taps = [params[slot, 2 + k : 3 + k, cols] for k in range(4)]
            bias = params[slot, 6:7, cols]
            conv = [
                bias
                + (
                    (line[r] * taps[0] + line[r + 1] * taps[1])
                    + (line[r + 2] * taps[2] + line[r + 3] * taps[3])
                )
                for r in range(rows)
            ]
            conv = jnp.concatenate(conv, axis=0).astype(BF16)
            both = []
            for b in range(2):
                block = 2 * n + b
                gate = jnp.concatenate(
                    [
                        w_out[slot, block, TILE:REST, q * TILE : (q + 1) * TILE]
                        for q in range(4)
                    ],
                    axis=0,
                )
                both.append(
                    jnp.dot(conv[:, b * 128 : (b + 1) * 128], gate, preferred_element_type=F32)
                )
            pieces.append((conv, both))
        return pieces

    def recur(p, pieces):
        for n in (2 * p, 2 * p + 1):
            conv16, both = pieces[n % 2]
            for b in range(2):
                lo = n * TILE + b * 128
                cols = slice(lo, lo + 128)
                sub = lax.broadcasted_iota(jnp.int32, (8, 128), 0)
                head = sub == 0
                conv = conv16[:, b * 128 : (b + 1) * 128].astype(F32)
                recur_bias = params[slot, 7:8, cols]
                inject_bias = params[slot, 8:9, cols]
                speed = params[slot, 9:10, cols]
                local_state = []
                local_decay = []
                for r in range(rows):
                    here = slice(r * 8, (r + 1) * 8)
                    spike = spikes[slot, here, :]
                    y = speed * jnp.tanh(both[b][here, :128] + recur_bias) + (speed - spike)
                    t = jnp.tanh(y)
                    decay = jnp.exp(-y)
                    twice = t + t
                    root = t * lax.rsqrt(jnp.maximum(twice + twice * t, 1e-37))
                    value = conv[here]
                    update = root * (value + value * jnp.tanh(both[b][here, 128:] + inject_bias))
                    if r == 0:
                        local_state.append(update)
                        local_decay.append(decay)
                    else:
                        local_state.append(decay * local_state[-1] + update)
                        local_decay.append(decay * local_decay[-1])
                a = local_decay[-1]
                h = local_state[-1]
                for shift in (1, 2, 4):
                    far = sub < shift
                    a_back = jnp.where(far, 1.0, pltpu.roll(a, shift, axis=0))
                    h_back = jnp.where(far, 0.0, pltpu.roll(h, shift, axis=0))
                    h = a * h_back + h
                    a = a * a_back
                start = jnp.where(first, 0.0, state_in[slot, 0:8, cols])
                start = jnp.broadcast_to(start[7:8], (8, 128))
                ends = a * start + h
                state_out[slot, 0:8, cols] = ends
                carry = jnp.where(head, start, rolled(ends))
                states[:, cols] = jnp.concatenate(
                    [local_state[r] + local_decay[r] * carry for r in range(rows)], axis=0
                ).astype(BF16)

    def output(p, e):
        out = None
        for k in (2 * p, 2 * p + 1):
            part = jnp.dot(
                states[:, k * TILE : (k + 1) * TILE],
                w_out[slot, e, 0:TILE, k * TILE : (k + 1) * TILE],
                preferred_element_type=F32,
            )
            out = part if out is None else out + part
        return out

    mixed = [project(0), project(1)]
    pieces = [convolve(p, mixed[p]) for p in range(2)]
    recur(0, pieces[0])
    early = [output(0, e) for e in range(8)]
    recur(1, pieces[1])
    for e in range(8):
        cols = slice(e * TILE, (e + 1) * TILE)
        out = early[e] + output(1, e)
        hidden[:, cols] = (hidden[:, cols].astype(F32) + out).astype(BF16)


def stage_kernel(
    flags, fresh, passed, w_in, w_out, params, spikes, state_in, out, state_out, normed, states
):
    @pl.when(flags[0] == 1)
    def _():
        first = flags[2] == 1

        @pl.when(flags[1] == 1)
        def _():
            out[...] = fresh[...]

        @pl.when(flags[1] == 0)
        def _():
            out[...] = passed[...]

        def body(index, unused):
            layer(
                index ^ flags[3], first, w_in, w_out, params, spikes, state_in, state_out, out, normed, states
            )
            return unused

        lax.fori_loop(0, LAYERS, body, 0)


def run_stage(flags, fresh, passed, w_in, w_out, params, spikes, state):
    vmem = pl.BlockSpec(memory_space=pltpu.VMEM)
    flops = LAYERS * CHUNK * 2 * (2 * D * RW + 2 * RW * 128)
    return pl.pallas_call(
        stage_kernel,
        in_specs=[pl.BlockSpec(memory_space=pltpu.SMEM)] + [vmem] * 7,
        out_specs=[vmem, vmem],
        out_shape=[
            jax.ShapeDtypeStruct((CHUNK, D), BF16),
            jax.ShapeDtypeStruct((LAYERS, STATE, RW), F32),
        ],
        scratch_shapes=[pltpu.VMEM((CHUNK, D), BF16), pltpu.VMEM((CHUNK, RW), BF16)],
        compiler_params=pltpu.CompilerParams(vmem_limit_bytes=14 * 2**20),
        cost_estimate=pl.CostEstimate(
            flops=4 * flops, transcendentals=5 * LAYERS * CHUNK * RW, bytes_accessed=2**20
        ),
        name="stage",
    )(flags, fresh, passed, w_in, w_out, params, spikes, state)


def shifted(value, by):
    return lax.ppermute(value, "z", [(i, (i + by) % STAGES) for i in range(STAGES)])


def turned(value):
    rows = CHUNK // 8
    halves = value.shape[0] // CHUNK
    return value.reshape(halves, 8, rows, -1).swapaxes(1, 2).reshape(value.shape)


def unturned(value):
    rows = CHUNK // 8
    halves = value.shape[0] // CHUNK
    return value.reshape(halves, rows, 8, -1).swapaxes(1, 2).reshape(value.shape)


def local(
    tokens,
    layer_norm_scale,
    input_weight,
    filter_weight,
    filter_bias,
    recur_gate_weight,
    recur_gate_bias,
    input_gate_weight,
    input_gate_bias,
    decay_setting,
    spike_log_decay,
    output_weight,
):
    stage = lax.axis_index("z")
    row = lax.axis_index("y")
    column = lax.axis_index("fs")
    core = lax.axis_index("tp")
    where = jnp.stack([column, core]).astype(jnp.int32)
    half = jnp.asarray(0.5, BF16)

    gates = jnp.concatenate([recur_gate_weight[0], input_gate_weight[0]], axis=2) * half
    gates = jnp.concatenate([gates[:, q * 32 : (q + 1) * 32] for q in range(4)], axis=2)
    ins = input_weight[0].reshape(4, 2, TILE, RW)
    ins = lax.dynamic_index_in_dim(ins, core, 1, keepdims=False)

    small = jnp.concatenate(
        [
            layer_norm_scale.reshape(2, RW),
            filter_weight[0],
            filter_bias,
            0.5 * recur_gate_bias,
            0.5 * input_gate_bias,
            4.0 * jax.nn.softplus(-decay_setting),
            jnp.pad(spike_log_decay, ((0, 0), (0, RW - spike_log_decay.shape[1]))),
            jnp.zeros((5, RW), F32),
        ],
        axis=0,
    )

    block = 2 * column + core
    piece = lax.dynamic_slice(output_weight[0], (0, block * TILE), (RW, TILE))
    piece = jnp.concatenate([piece[k * TILE : (k + 1) * TILE] for k in range(4)], axis=1)
    piece = jnp.concatenate(
        [piece, lax.dynamic_index_in_dim(gates, block, 0, keepdims=False)], axis=0
    )
    one, three, low, high = ring_gather(piece, "y")
    near = jnp.stack([one, three])
    far = jnp.concatenate([low, high], axis=0)
    in_one, in_three, in_low, in_high = ring_gather(ins, "y")
    near_all = ring_gather(near, "fs")
    far_all = ring_gather(far, "fs")
    near_blocks = jnp.concatenate([near, *near_all], axis=0)
    far_blocks = jnp.stack(
        [far, far_all[0], far_all[1], jnp.concatenate([far_all[2], far_all[3]], axis=0)]
    )
    in_two = jnp.concatenate([in_low, in_high], axis=0)
    w_out = load(
        out_kernel,
        REST,
        where,
        output_weight,
        gates,
        near_blocks,
        crossed(near_blocks, "tp", 1),
        far_blocks,
        crossed(far_blocks, "tp", 1),
    )
    w_in = load(
        in_kernel,
        TILE,
        where,
        input_weight,
        in_one,
        crossed(in_one, "tp", 1),
        in_three,
        crossed(in_three, "tp", 1),
        in_two,
        crossed(in_two, "tp", 1),
    )

    params = jnp.stack(
        [small, crossed(small, "y", 1), crossed(small, "y", 2), crossed(small, "y", 3)]
    )
    spikes = params[:, 10, : tokens.shape[2]]
    spikes = spikes.reshape(LAYERS, 2, 8, CHUNK // 8).swapaxes(2, 3).reshape(LAYERS, 2, CHUNK, 1)
    spikes = jnp.broadcast_to(spikes, (LAYERS, 2, CHUNK, 128))
    spikes = [spikes[:, 0], spikes[:, 1]]

    mine = turned(tokens[0, 0])
    batches = [mine] + [shifted(mine, -by) for by in range(1, STAGES)]

    chunks = 2 * STAGES
    steps = chunks + 2 * (STAGES - 1)
    state = jnp.zeros((LAYERS, STATE, RW), F32)
    results = []
    received = []
    for t in range(steps):
        chunk = t - 2 * stage
        active = (chunk >= 0) & (chunk < chunks)
        flags = jnp.stack([active, stage == 0, jnp.asarray(t % 2 == 0), row]).astype(jnp.int32)
        batch = batches[min(t // 2, STAGES - 1)]
        fresh = batch[:CHUNK] if t % 2 == 0 else batch[CHUNK:]
        passed = received[t - 2] if t >= 2 else fresh
        result, state = run_stage(
            flags, fresh, passed, w_in, w_out, params, spikes[t % 2], state
        )
        results.append(result)
        received.append(shifted(result, 1) if t < steps - 2 else None)

    last = 2 * (STAGES - 1)
    halves = []
    for j in range(2):
        home = [received[last + j]]
        home += [shifted(results[last + 2 * m + j], -(STAGES - 1 - m)) for m in range(1, STAGES - 1)]
        home += [results[last + 2 * (STAGES - 1) + j]]
        chosen = home[0]
        for m in range(1, STAGES):
            chosen = jnp.where(stage == m, home[m], chosen)
        halves.append(chosen)
    return unturned(jnp.concatenate(halves, axis=0))[None, None]


def solution(mesh):
    split = Mesh(mesh.devices.reshape(4, 4, 4, 2), ("z", "y", "fs", "tp"))
    layers = ("z", "y")
    placed = (
        P(layers, ("fs", "tp"), None, None),
        P(layers, None),
        P(layers, None, None),
        P(layers, None, None),
        P(layers, None),
        P(layers, None, None, None),
        P(layers, None),
        P(layers, None, None, None),
        P(layers, None),
        P(layers, None),
        P(layers, None),
        P(layers, None, None),
    )
    return jax.shard_map(
        local,
        mesh=split,
        in_specs=placed,
        out_specs=P(layers, ("fs", "tp"), None, None),
        check_vma=False,
    )
```
